32 devices in a mesh: ep: 8 (over z, x), tp: 4 (over y, core).
Axes of the slice: x: 2, y: 2, z: 4, core: 2. Of those that a mesh axis runs over, the one named last changes fastest.
Arguments:
- queries: bfloat16 [2048, 2048], P('ep', 'tp'), may hold values from -9 to 9
- keys: bfloat16 [2048, 2048], P('ep', 'tp'), may hold values from -9 to 9
- values: bfloat16 [2048, 2048], P('ep', 'tp'), may hold values from -6 to 6
- lambdas: float32 [16], P('tp'), may hold values from 0.3 to 0.8
- head_gain: float32 [128], replicated, may hold values from 0.1 to 1.9
- moe_input: bfloat16 [4096, 2048], P('ep'), may hold values from -6 to 6
- ffn_gain: float32 [2048], replicated, may hold values from 0.1 to 1.9
- group_router: bfloat16 [2048, 4], replicated, may hold values from -0.125 to 0.125
- expert_router: bfloat16 [2048, 8], replicated, may hold values from -0.125 to 0.125
- routes: int32 [4096, 2], P('ep'), may hold values from 0 to 7, as said below
- w_gate: bfloat16 [8, 2048, 1024], P('ep', None, 'tp'), may hold values from -0.125 to 0.125
- w_up: bfloat16 [8, 2048, 1024], P('ep', None, 'tp'), may hold values from -0.125 to 0.125
- w_down: bfloat16 [8, 1024, 2048], P('ep', 'tp'), may hold values from -0.1875 to 0.1875
Outputs:
- attn_out: bfloat16 [2048, 2048], P('ep', 'tp')
- moe_out: bfloat16 [4096, 2048], P(('ep', 'tp'))
The draws below stay inside these ranges and needn't reach their ends.
Inputs may be any that keep to these rules, and one draw needn't show every extreme that they name: `routes`: in each aligned block of 128 rows (the rows of one device) every expert is named by exactly 32 rows and every group by the same number of rows; a row's two experts differ and lie in one group of 2 consecutive expert numbers.
All inputs are finite; a program needn't handle non-finite values.
Results may differ from the reference program's by a relative error of at most 0.015.
Values may be sent and summed in bfloat16 or wider, within the bound.
A program may use at most 128 MiB of HBM per device.

```python
import jax
import jax.numpy as jnp
from jax import lax

D = 2048
HEADS = 16
QK_DIM = 64
V_DIM = 128
FF = 1024
GROUPS = 4
TOPK = 2
ROWS = 128
EXPERTS = 8
GROUP_SIZE = 2
FF_PART = 256
TOK_A = 2048
TOK_B = 4096
N_TP = 4


def draw_queries(key, part):
    shape = (TOK_A, HEADS * 2 * QK_DIM)
    drawn = jnp.clip(1.3 * jax.random.normal(jax.random.fold_in(key, 1), shape, jnp.float32), -6.0, 6.0)
    return drawn.astype(jnp.bfloat16)


def draw_keys(key, part):
    shape = (TOK_A, HEADS * 2 * QK_DIM)
    drawn = jnp.clip(1.3 * jax.random.normal(jax.random.fold_in(key, 2), shape, jnp.float32), -6.0, 6.0)
    return drawn.astype(jnp.bfloat16)


def draw_routes(key, part):
    block_count = TOK_B // ROWS
    per_group = ROWS // GROUPS
    block_keys = jax.random.split(jax.random.fold_in(key, 11), block_count)

    def one_block(block_key):
        place_key, group_key, expert_key, order_key = jax.random.split(block_key, 4)
        places = jax.random.permutation(place_key, ROWS)
        group_index = places // per_group
        inner_index = places % per_group
        first_pick = inner_index % GROUP_SIZE
        shift_amount = 1 + inner_index // GROUP_SIZE % (GROUP_SIZE - 1)
        second_pick = (first_pick + shift_amount) % GROUP_SIZE
        group_labels = jax.random.permutation(group_key, GROUPS)[group_index]
        expert_orders = jax.vmap(lambda inner_key: jax.random.permutation(inner_key, GROUP_SIZE))(jax.random.split(expert_key, GROUPS))
        first_expert = expert_orders[group_index, first_pick]
        second_expert = expert_orders[group_index, second_pick]
        flips = jax.random.randint(order_key, (ROWS,), 0, 2)
        lead_expert = jnp.where(flips == 1, second_expert, first_expert)
        tail_expert = jnp.where(flips == 1, first_expert, second_expert)
        base_number = group_labels * GROUP_SIZE
        return jnp.stack([base_number + lead_expert, base_number + tail_expert], axis=1)
    return jax.vmap(one_block)(block_keys).reshape(TOK_B, TOPK).astype(jnp.int32)


def shard_levels(key, extent, cuts, low, largest):
    level = 1.0
    for position, parts in cuts:
        draws = jax.random.uniform(jax.random.fold_in(jax.random.fold_in(key, 6), position), (parts,), jnp.float32, low / len(cuts), largest / len(cuts))
        level = level * jnp.repeat(jnp.exp(draws), extent[position] // parts).reshape((-1,) + (1,) * (len(extent) - 1 - position))
    return level


def centred(key, dims, spread, limit, shards=(), kind=jnp.bfloat16):
    entries = spread * jax.random.normal(key, dims, jnp.float32)
    if shards:
        entries = entries * shard_levels(key, dims, shards, -0.22, 0.18)
    return jnp.clip(entries, -limit, limit).astype(kind)


def setup_inputs(seed: int = 0) -> dict:
    key_list = jax.random.split(jax.random.key(seed), 14)
    queries = draw_queries(jax.random.fold_in(key_list[13], 71), 0)
    keys = draw_keys(jax.random.fold_in(key_list[13], 71), 0)
    values = centred(key_list[2], (TOK_A, HEADS * V_DIM), 1.0, 6.0, ((0, 8), (1, 4)))
    lambdas = jnp.clip(0.3 + 0.5 * jax.random.uniform(key_list[3], (HEADS,), jnp.float32) ** shard_levels(key_list[3], (HEADS,), ((0, 4),), -0.2, 0.2), 0.3, 0.8)
    head_gain = jnp.clip(1.0 + 0.18 * jax.random.normal(key_list[4], (V_DIM,), jnp.float32), 0.1, 1.9)
    moe_input = centred(key_list[5], (TOK_B, D), 1.0, 6.0, ((0, 8),))
    ffn_gain = jnp.clip(1.0 + 0.18 * jax.random.normal(key_list[6], (D,), jnp.float32), 0.1, 1.9)
    group_router = centred(key_list[7], (D, GROUPS), D ** -0.5, 0.125)
    expert_router = centred(key_list[8], (D, EXPERTS), D ** -0.5, 0.125)
    routes = draw_routes(jax.random.fold_in(key_list[13], 71), 0)
    w_gate = centred(key_list[10], (EXPERTS, D, FF), D ** -0.5, 0.125, ((0, 8), (2, 4)))
    w_up = centred(key_list[11], (EXPERTS, D, FF), D ** -0.5, 0.125, ((0, 8), (2, 4)))
    w_down = centred(key_list[12], (EXPERTS, FF, D), FF ** -0.5, 0.1875, ((0, 8), (1, 4)))
    return {"queries": queries, "keys": keys, "values": values, "lambdas": lambdas, "head_gain": head_gain, "moe_input": moe_input, "ffn_gain": ffn_gain, "group_router": group_router, "expert_router": expert_router, "routes": routes, "w_gate": w_gate, "w_up": w_up, "w_down": w_down}


norm_eps = 1e-06

def rms_scaled(rows, gain):
    widened = rows.astype(jnp.float32)
    return widened * lax.rsqrt(lax.optimization_barrier(jnp.mean(widened * widened, axis=-1, keepdims=True)) + norm_eps) * gain

def route_gates(normed, own_routes, group_router, expert_router):
    group_count = group_router.shape[1]
    expert_count = expert_router.shape[1]
    group_logits = jnp.dot(normed, group_router, preferred_element_type=jnp.float32)
    expert_logits = jnp.dot(normed, expert_router, preferred_element_type=jnp.float32)
    chosen = own_routes[:, 0] // (expert_count // group_count)
    group_mask = jnp.arange(group_count, dtype=jnp.int32)[None, :] == chosen[:, None]
    own_logit = lax.optimization_barrier(jnp.sum(jnp.where(group_mask, group_logits, 0.0), axis=-1, keepdims=True))
    group_share = 1.0 / lax.optimization_barrier(jnp.sum(jnp.exp(group_logits - own_logit), axis=-1))
    expert_mask = jnp.arange(expert_count, dtype=jnp.int32)[None, None, :] == own_routes[:, :, None]
    picked = lax.optimization_barrier(jnp.sum(jnp.where(expert_mask, expert_logits[:, None, :], 0.0), axis=-1))
    return group_share[:, None] * jax.nn.sigmoid(picked - picked[:, ::-1])

def attention_part(queries, keys, values, lambdas, head_gain):
    row_count = queries.shape[0]
    query_heads = queries.reshape(row_count, HEADS, 2, QK_DIM).astype(jnp.float32).transpose(1, 0, 2, 3)
    key_heads = keys.reshape(row_count, HEADS, 2, QK_DIM).astype(jnp.float32).transpose(1, 0, 2, 3)
    value_heads = values.reshape(row_count, HEADS, V_DIM).transpose(1, 0, 2)
    positions = jnp.arange(row_count, dtype=jnp.int32)
    allowed = positions[None, :] <= positions[:, None]

    def one_head(pack):
        query_one, key_one, value_one, weight_one = pack
        scores = jnp.einsum('qmd,kmd->mqk', query_one, key_one) * QK_DIM ** (-0.5)
        scores = jnp.where(allowed, scores, -jnp.inf)
        maxima = lax.optimization_barrier(jnp.max(scores, axis=-1, keepdims=True))
        exp_terms = jnp.where(allowed, jnp.exp(scores - maxima), 0.0)
        shares = exp_terms / lax.optimization_barrier(jnp.sum(exp_terms, axis=-1, keepdims=True))
        mixed = (shares[0] - weight_one * shares[1]).astype(jnp.bfloat16)
        return jnp.dot(mixed, value_one, preferred_element_type=jnp.float32)
    heads_out = lax.map(one_head, (query_heads, key_heads, value_heads, lambdas))
    normed = rms_scaled(heads_out, head_gain).astype(jnp.bfloat16)
    return normed.transpose(1, 0, 2).reshape(row_count, HEADS * V_DIM)

def expert_part(moe_input, ffn_gain, group_router, expert_router, routes, w_gate, w_up, w_down):
    normed = rms_scaled(moe_input, ffn_gain).astype(jnp.bfloat16)
    gates = route_gates(normed, routes, group_router, expert_router)
    flat_routes = routes.reshape(-1)
    sorted_order = jnp.argsort(flat_routes, stable=True).astype(jnp.int32)
    per_expert = flat_routes.shape[0] // EXPERTS
    sorted_rows = normed[sorted_order // 2].reshape(EXPERTS, per_expert, D)

    def one_expert(pack):
        expert_rows, gate_weight, up_weight, down_weight = pack
        gate_part = jnp.dot(expert_rows, gate_weight, preferred_element_type=jnp.float32)
        up_part = jnp.dot(expert_rows, up_weight, preferred_element_type=jnp.float32)
        hidden = (jax.nn.silu(gate_part) * up_part).astype(jnp.bfloat16)
        pieces = hidden.reshape(per_expert, N_TP, FF_PART).astype(jnp.float32)
        down_parts = down_weight.reshape(N_TP, FF_PART, D).astype(jnp.float32)
        partial_value = jnp.einsum('nsf,sfd->snd', pieces, down_parts).astype(jnp.bfloat16)
        partial_value = lax.optimization_barrier(partial_value)
        return lax.optimization_barrier(jnp.sum(partial_value.astype(jnp.float32), axis=0)).astype(jnp.bfloat16)
    outputs = lax.map(one_expert, (sorted_rows, w_gate, w_up, w_down)).reshape(-1, D)
    placed = jnp.zeros_like(outputs).at[sorted_order].set(outputs)
    per_token = placed.reshape(-1, 2, D).astype(jnp.float32)
    return lax.optimization_barrier(jnp.sum(per_token * gates[..., None], axis=1)).astype(jnp.bfloat16)

def reference(queries, keys, values, lambdas, head_gain, moe_input, ffn_gain, group_router, expert_router, routes, w_gate, w_up, w_down):
    attn_out = attention_part(queries, keys, values, lambdas, head_gain)
    moe_out = expert_part(moe_input, ffn_gain, group_router, expert_router, routes, w_gate, w_up, w_down)
    return (attn_out, moe_out)
```

```python
import functools
import math

import jax
import jax.numpy as jnp
from jax import lax
from jax.experimental import pallas as pl
from jax.experimental.pallas import tpu as pltpu
from jax.sharding import PartitionSpec as P

norm_eps = 1e-06
masked_score = -1e30


def rms_scaled(rows, gain):
    widened = rows.astype(jnp.float32)
    return (
        widened * lax.rsqrt(jnp.mean(widened * widened, axis=-1, keepdims=True) + norm_eps) * gain
    )


def score_block(query_heads, key_rows, score_scale):
    key_heads = key_rows.reshape(key_rows.shape[0], query_heads.shape[1], 2, query_heads.shape[3])
    return (
        jnp.einsum("qhmd,khmd->hmqk", query_heads, key_heads, preferred_element_type=jnp.float32)
        * score_scale
    )


def route_gates(normed, own_routes, group_router, expert_router):
    group_count = group_router.shape[1]
    expert_count = expert_router.shape[1]
    group_logits = jnp.dot(normed, group_router, preferred_element_type=jnp.float32)
    expert_logits = jnp.dot(normed, expert_router, preferred_element_type=jnp.float32)
    chosen = own_routes[:, 0] // (expert_count // group_count)
    group_mask = jnp.arange(group_count, dtype=jnp.int32)[None, :] == chosen[:, None]
    own_logit = jnp.sum(jnp.where(group_mask, group_logits, 0.0), axis=-1, keepdims=True)
    group_share = 1.0 / jnp.sum(jnp.exp(group_logits - own_logit), axis=-1)
    expert_mask = jnp.arange(expert_count, dtype=jnp.int32)[None, None, :] == own_routes[:, :, None]
    picked = jnp.sum(jnp.where(expert_mask, expert_logits[:, None, :], 0.0), axis=-1)
    return group_share[:, None] * jax.nn.sigmoid(picked - picked[:, ::-1])


def slot_places(own_routes, expert_count, capacity):
    flat_routes = own_routes.reshape(-1)
    one_hot = (flat_routes[:, None] == jnp.arange(expert_count, dtype=jnp.int32)[None, :]).astype(
        jnp.int32
    )
    earlier = jnp.cumsum(one_hot, axis=0) - one_hot
    return flat_routes * capacity + jnp.sum(earlier * one_hot, axis=1)


def dispatch_rows(normed_rows, own_routes, expert_count, capacity):
    places = slot_places(own_routes, expert_count, capacity)
    owners = jnp.arange(places.shape[0], dtype=jnp.int32) // 2
    holder = jnp.zeros((expert_count * capacity,), jnp.int32).at[places].set(owners)
    return normed_rows[holder].reshape(expert_count, capacity, normed_rows.shape[1])


def local(
    queries,
    keys,
    values,
    lambdas,
    head_gain,
    moe_input,
    ffn_gain,
    group_router,
    expert_router,
    routes,
    w_gate,
    w_up,
    w_down,
):
    query_count = queries.shape[0]
    heads_here = lambdas.shape[0]
    value_width = values.shape[1] // heads_here
    qk_width = queries.shape[1] // (2 * heads_here)
    query_heads = queries.reshape(query_count, heads_here, 2, qk_width)
    score_scale = qk_width ** (-0.5)
    query_first = lax.axis_index("ep") * query_count
    query_pos = query_first + jnp.arange(query_count, dtype=jnp.int32)
    query_last = query_first + query_count - 1
    stats_start = (
        jnp.full((heads_here, 2, query_count), masked_score, jnp.float32),
        jnp.zeros((heads_here, 2, query_count), jnp.float32),
    )
    key_shard = lax.all_gather(keys, "ep", axis=0, tiled=True)
    block_rows = math.gcd(key_shard.shape[0], 512)

    def stats_sweep_step(number, current):
        offset = number * block_rows

        def stats_compute(running):
            maxima, totals = running
            key_pos = offset + jnp.arange(block_rows, dtype=jnp.int32)
            allowed = key_pos[None, :] <= query_pos[:, None]
            key_block = lax.dynamic_slice_in_dim(key_shard, offset, block_rows, 0)
            scores = jnp.where(
                allowed, score_block(query_heads, key_block, score_scale), masked_score
            )
            new_max = jnp.maximum(maxima, jnp.max(scores, axis=-1))
            weights = jnp.where(allowed, jnp.exp(scores - new_max[..., None]), 0.0)
            return (new_max, totals * jnp.exp(maxima - new_max) + jnp.sum(weights, axis=-1))

        return lax.cond(offset <= query_last, stats_compute, lambda running: running, current)

    maxima, totals = lax.fori_loop(
        0, key_shard.shape[0] // block_rows, stats_sweep_step, stats_start
    )
    value_key_shard = lax.all_gather(keys, "ep", axis=0, tiled=True)
    value_shard = lax.all_gather(values, "ep", axis=0, tiled=True)
    value_block_rows = math.gcd(value_key_shard.shape[0], 512)

    def value_sweep_step(number, current):
        offset = number * value_block_rows

        def value_compute(running):
            key_pos = offset + jnp.arange(value_block_rows, dtype=jnp.int32)
            allowed = key_pos[None, :] <= query_pos[:, None]
            key_block = lax.dynamic_slice_in_dim(value_key_shard, offset, value_block_rows, 0)
            scores = score_block(query_heads, key_block, score_scale)
            shares = (
                jnp.where(allowed, jnp.exp(scores - maxima[..., None]), 0.0) / totals[..., None]
            )
            mixed = (shares[:, 0] - lambdas[:, None, None] * shares[:, 1]).astype(jnp.bfloat16)
            value_rows = lax.dynamic_slice_in_dim(value_shard, offset, value_block_rows, 0).reshape(
                value_block_rows, heads_here, value_width
            )
            return running + jnp.einsum(
                "hqk,khd->hqd", mixed, value_rows, preferred_element_type=jnp.float32
            )

        return lax.cond(offset <= query_last, value_compute, lambda running: running, current)

    heads_out = lax.fori_loop(
        0,
        value_key_shard.shape[0] // value_block_rows,
        value_sweep_step,
        jnp.zeros((heads_here, query_count, value_width), jnp.float32),
    )
    attn_out = rms_scaled(heads_out, head_gain).astype(jnp.bfloat16)
    attn_out = attn_out.transpose(1, 0, 2).reshape(query_count, heads_here * value_width)
    tp_count = lax.axis_size("tp")
    tp_index = lax.axis_index("tp")
    own_count = routes.shape[0] // tp_count
    expert_count = expert_router.shape[1]
    capacity = 2 * own_count // expert_count
    model_width = moe_input.shape[1]
    own_routes = lax.dynamic_slice_in_dim(routes, tp_index * own_count, own_count, 0)
    gate_local = w_gate[0]
    up_local = w_up[0]
    down_local = w_down[0]
    own_input = lax.dynamic_slice_in_dim(moe_input, tp_index * own_count, own_count, 0)
    normed = rms_scaled(own_input, ffn_gain).astype(jnp.bfloat16)
    packed = dispatch_rows(normed, own_routes, expert_count, capacity)
    arrived = lax.all_to_all(packed, "ep", split_axis=0, concat_axis=0, tiled=True)
    arrived_rows = lax.all_gather(arrived.reshape(-1, model_width), "tp", axis=0, tiled=True)
    gate_part = jnp.dot(arrived_rows, gate_local, preferred_element_type=jnp.float32)
    up_part = jnp.dot(arrived_rows, up_local, preferred_element_type=jnp.float32)
    hidden = (jax.nn.silu(gate_part) * up_part).astype(jnp.bfloat16)
    summed = lax.psum_scatter(
        jnp.dot(hidden, down_local, preferred_element_type=jnp.float32).astype(jnp.bfloat16),
        "tp",
        scatter_dimension=0,
        tiled=True,
    )
    homed = lax.all_to_all(
        summed.reshape(expert_count, capacity, model_width),
        "ep",
        split_axis=0,
        concat_axis=0,
        tiled=True,
    )
    places = slot_places(own_routes, expert_count, capacity)
    returned = homed.reshape(expert_count * capacity, model_width)[places].reshape(
        own_count, 2, model_width
    )
    gates = route_gates(normed, own_routes, group_router, expert_router)
    moe_out = jnp.sum(returned.astype(jnp.float32) * gates[..., None], axis=1).astype(jnp.bfloat16)
    return (attn_out, moe_out)


class Copies:
    def __init__(self, send_sems, recv_sems):
        self.send_sems = send_sems
        self.recv_sems = recv_sems
        self.made = []

    def new(self, source, target, device):
        number = len(self.made)
        copy = pltpu.make_async_remote_copy(
            src_ref=source,
            dst_ref=target,
            send_sem=self.send_sems.at[number],
            recv_sem=self.recv_sems.at[number],
            device_id=device,
            device_id_type=pl.DeviceIdType.MESH,
        )
        copy.start()
        self.made.append(copy)
        return copy

    def drain(self):
        for copy in self.made:
            copy.wait_send()


def fused_kernel(
    groups,
    score_scale,
    queries,
    keys,
    values,
    lambdas,
    head_gain,
    moe_input,
    ffn_gain,
    router,
    routes,
    w_gate,
    w_up,
    w_down,
    attn_out,
    moe_out,
    own_rows,
    packed,
    rows,
    gate_w,
    up_w,
    down_w,
    half_out,
    half_in,
    sums,
    corner_out,
    corner_in,
    side_out,
    side_in,
    done,
    returned,
    q_all,
    k_all,
    v_all,
    heads_done,
    heads_back,
    local_sems,
    send_sems,
    recv_sems,
):
    own_count, model_width = own_rows.shape
    chunk = own_count // groups
    half = chunk // 2
    token_block, head_width = q_all.shape[1:]
    ep = lax.axis_index("ep")
    tp = lax.axis_index("tp")
    plane, member = ep // 2, ep % 2
    row, core = tp // 2, tp % 2
    member_peer = (plane * 2 + (1 - member), tp)
    row_peer = (ep, (1 - row) * 2 + core)
    core_peer = (ep, row * 2 + (1 - core))
    ahead = [(plane + step) % groups for step in range(groups)]
    behind = [(plane + groups - step) % groups for step in range(groups)]

    def at_plane(number):
        return (number * 2 + member, tp)

    def head_columns(ref, number):
        return ref.at[:, pl.ds(pl.multiple_of(number * head_width, head_width), head_width)]

    loads = []
    for source, target in (
        (moe_input.at[pl.ds(pl.multiple_of(tp * own_count, own_count), own_count)], own_rows),
        (head_columns(queries, plane), q_all.at[plane]),
        (head_columns(keys, plane), k_all.at[ep]),
        (head_columns(values, plane), v_all.at[ep]),
        (w_gate.at[0], gate_w),
        (w_up.at[0], up_w),
        (w_down.at[0], down_w),
    ):
        load = pltpu.make_async_copy(source, target, local_sems.at[len(loads)])
        load.start()
        loads.append(load)

    barrier = pltpu.get_barrier_semaphore()
    partners = [member_peer, row_peer, core_peer] + [at_plane(p) for p in ahead[1:]]
    for partner in partners:
        pl.semaphore_signal(
            barrier, inc=1, device_id=partner, device_id_type=pl.DeviceIdType.MESH
        )

    own_routes = routes[pl.ds(pl.multiple_of(tp * own_count, own_count), own_count), :]
    lead = own_routes[:, 0:1]
    lane = lax.broadcasted_iota(jnp.int32, (own_count, own_count), 1)
    sub = lax.broadcasted_iota(jnp.int32, (own_count, own_count), 0)
    turned = plane + lane
    lane_group = jnp.where(turned >= groups, turned - groups, turned)
    in_group = (lead >= lane_group * 2) & (lead < lane_group * 2 + 2) & (lane < groups)
    one_hot = jnp.where(in_group, 1.0, 0.0)
    below = jnp.where(lane < sub, 1.0, 0.0).astype(jnp.bfloat16)
    earlier = jnp.dot(below, one_hot.astype(jnp.bfloat16), preferred_element_type=jnp.float32)
    lane_start = (lane * chunk).astype(jnp.float32)
    place = jnp.sum(one_hot * (earlier + lane_start), axis=1, keepdims=True)
    slots = jnp.where(place == lane.astype(jnp.float32), 1.0, 0.0).astype(jnp.bfloat16)

    loads[0].wait()
    widened = own_rows[...].astype(jnp.float32)
    normed = (
        widened
        * lax.rsqrt(jnp.mean(widened * widened, axis=-1, keepdims=True) + norm_eps)
        * ffn_gain[...]
    ).astype(jnp.bfloat16)
    by_group = lax.dot_general(
        slots, normed, (((0,), (0,)), ((), ())), preferred_element_type=jnp.float32
    ).astype(jnp.bfloat16)
    rows[0, 0:chunk, :] = by_group[0:chunk]
    for step in range(1, groups):
        packed[step] = by_group[step * chunk : (step + 1) * chunk]

    pl.semaphore_wait(barrier, len(partners))
    copies = Copies(send_sems, recv_sems)

    def slot(step, number):
        return rows.at[step, pl.ds(number * chunk, chunk)]

    arriving = [None] * groups
    for step in range(1, groups):
        arriving[step] = copies.new(packed.at[step], slot(step, 0), at_plane(ahead[step]))
    kv_arriving = [None] * groups
    q_arriving = []

    def send_heads(step):
        target = at_plane(ahead[step])
        kv_arriving[step] = [
            copies.new(head_columns(keys, ahead[step]), k_all.at[ep], target),
            copies.new(head_columns(values, ahead[step]), v_all.at[ep], target),
        ]
        q_arriving.append(
            copies.new(head_columns(queries, ahead[step]), q_all.at[plane], target)
        )

    first = [None] * groups
    second = [None] * groups
    third = [None] * groups
    crossed = [None] * groups
    corner = [None] * groups
    sides = [None] * groups
    homed = []
    kv_crossed = []

    def spread(step):
        if arriving[step] is not None:
            arriving[step].wait_recv()
        first[step] = [
            copies.new(slot(step, 0), slot(step, 1), member_peer),
            copies.new(slot(step, 0), slot(step, 2), row_peer),
        ]
        third[step] = [copies.new(slot(step, 0), slot(step, groups_in_half), core_peer)]

    def forward(step):
        upper = pl.ds(3 * chunk, half)
        lower = pl.ds(3 * chunk + half, half)
        first[step][0].wait_recv()
        to_row = copies.new(
            rows.at[step, pl.ds(chunk, half)], rows.at[step, upper], row_peer
        )
        third[step].append(copies.new(slot(step, 1), slot(step, 5), core_peer))
        first[step][1].wait_recv()
        to_member = copies.new(
            rows.at[step, pl.ds(2 * chunk + half, half)], rows.at[step, lower], member_peer
        )
        third[step].append(copies.new(slot(step, 2), slot(step, 6), core_peer))
        second[step] = [to_row, to_member]

    def compute(step):
        for copy in second[step]:
            copy.wait_recv()
        third[step].append(copies.new(slot(step, 3), slot(step, 7), core_peer))
        for copy in third[step]:
            copy.wait_recv()
        if step == 0:
            for load in loads[4:]:
                load.wait()
        block = rows[step]
        logits = jnp.dot(block, router[...], preferred_element_type=jnp.float32)
        column = lax.broadcasted_iota(jnp.int32, logits.shape, 1)

        def pick(number):
            return jnp.sum(jnp.where(column == number, logits, 0.0), axis=1, keepdims=True)

        own_group = pick(plane)
        terms = jnp.where(column < groups, jnp.exp(logits - own_group), 0.0)
        share = 1.0 / jnp.sum(jnp.where(column < groups, terms, 0.0), axis=1, keepdims=True)
        gap = pick(groups + ep) - pick(groups + plane * 2 + (1 - member))
        gates = share / (1.0 + jnp.exp(-gap))
        gate_part = jnp.dot(block, gate_w[...], preferred_element_type=jnp.float32)
        up_part = jnp.dot(block, up_w[...], preferred_element_type=jnp.float32)
        hidden = (gate_part / (1.0 + jnp.exp(-gate_part)) * up_part).astype(jnp.bfloat16)
        out = jnp.dot(hidden, down_w[...], preferred_element_type=jnp.float32) * gates
        half_out[step] = out[4 * chunk :].astype(jnp.bfloat16)
        sums[step] = out[: 4 * chunk]
        crossed[step] = copies.new(half_out.at[step], half_in.at[step], core_peer)

    def reduce_corner(step):
        crossed[step].wait_recv()
        total = sums[step] + half_in[step].astype(jnp.float32)
        sums[step] = total
        corner_out[step] = total[3 * chunk :].astype(jnp.bfloat16)
        corner[step] = [
            copies.new(
                corner_out.at[step, pl.ds(0, half)], corner_in.at[step, pl.ds(0, half)], row_peer
            ),
            copies.new(
                corner_out.at[step, pl.ds(half, half)],
                corner_in.at[step, pl.ds(half, half)],
                member_peer,
            ),
        ]

    def reduce_sides(step):
        for copy in corner[step]:
            copy.wait_recv()
        added = corner_in[step].astype(jnp.float32)
        total = sums[step]
        side_out[step, 0:half, :] = (total[chunk : chunk + half] + added[:half]).astype(
            jnp.bfloat16
        )
        side_out[step, half : half + chunk, :] = total[chunk + half : 2 * chunk + half].astype(
            jnp.bfloat16
        )
        side_out[step, half + chunk :, :] = (total[2 * chunk + half : 3 * chunk] + added[half:]).astype(
            jnp.bfloat16
        )
        sides[step] = [
            copies.new(
                side_out.at[step, pl.ds(0, chunk)], side_in.at[step, pl.ds(0, chunk)], member_peer
            ),
            copies.new(
                side_out.at[step, pl.ds(chunk, chunk)],
                side_in.at[step, pl.ds(chunk, chunk)],
                row_peer,
            ),
        ]

    def finish(step):
        for copy in sides[step]:
            copy.wait_recv()
        arrived = side_in[step].astype(jnp.float32)
        total = (sums[step][:chunk] + arrived[:chunk] + arrived[chunk:]).astype(jnp.bfloat16)
        if step == 0:
            returned[0] = total
        else:
            done[step] = total
            homed.append(copies.new(done.at[step], returned.at[step], at_plane(behind[step])))

    def cross_heads(step):
        if step == 0:
            loads[2].wait()
            loads[3].wait()
        else:
            for copy in kv_arriving[step]:
                copy.wait_recv()
        block = behind[step] * 2 + member
        kv_crossed.append(copies.new(k_all.at[block], k_all.at[block], member_peer))
        kv_crossed.append(copies.new(v_all.at[block], v_all.at[block], member_peer))

    def ready_heads():
        loads[1].wait()
        for copy in q_arriving + kv_crossed:
            copy.wait_recv()

    back = []
    weight = lambdas[plane]
    factor = score_scale * math.log2(math.e)

    def attend(number):
        query = q_all[number]
        lanes = lax.broadcasted_iota(jnp.int32, query.shape, 1)
        nothing = jnp.zeros_like(query)
        maps = [
            jnp.where(lanes < head_width // 2, query, nothing),
            jnp.where(lanes >= head_width // 2, query, nothing),
        ]
        ends = [2 * number, 2 * number + 2]
        parts = [(0, ends[0])] if number else []
        parts.append((ends[0], ends[1]))
        key_parts = [k_all[a:b].reshape((b - a) * token_block, head_width) for a, b in parts]
        value_parts = [v_all[a:b].reshape((b - a) * token_block, head_width) for a, b in parts]
        mixed = [None] * len(parts)
        for index, part_query in enumerate(maps):
            scores = [
                lax.dot_general(
                    part_query, k, (((1,), (1,)), ((), ())), preferred_element_type=jnp.float32
                )
                for k in key_parts
            ]
            at = lax.broadcasted_iota(jnp.int32, scores[-1].shape, 1)
            own = lax.broadcasted_iota(jnp.int32, scores[-1].shape, 0) + member * token_block
            scores[-1] = jnp.where(at <= own, scores[-1], masked_score)
            maxima = functools.reduce(
                jnp.maximum, [jnp.max(s, axis=1, keepdims=True) for s in scores]
            )
            terms = [jnp.exp2((s - maxima) * factor) for s in scores]
            total = sum(jnp.sum(t, axis=1, keepdims=True) for t in terms)
            share = 1.0 / total if index == 0 else -weight / total
            for place_number, t in enumerate(terms):
                piece = t * share
                if index:
                    piece = mixed[place_number] + piece
                mixed[place_number] = piece
        heads = sum(
            jnp.dot(w.astype(jnp.bfloat16), v, preferred_element_type=jnp.float32)
            for w, v in zip(mixed, value_parts)
        )
        scaled = (
            heads
            * lax.rsqrt(jnp.mean(heads * heads, axis=-1, keepdims=True) + norm_eps)
            * head_gain[...]
        )
        heads_done[number] = scaled.astype(jnp.bfloat16)

    def send_attended():
        for step in range(1, groups):
            back.append(
                copies.new(
                    heads_done.at[ahead[step]], heads_back.at[plane], at_plane(ahead[step])
                )
            )

    groups_in_half = 4
    spread(0)
    cross_heads(0)
    for step in range(1, groups):
        send_heads(step)
    forward(0)
    spread(1)
    compute(0)
    forward(1)
    spread(2)
    reduce_corner(0)
    compute(1)
    cross_heads(1)
    forward(2)
    reduce_sides(0)
    spread(3)
    reduce_corner(1)
    compute(2)
    cross_heads(2)
    forward(3)
    finish(0)
    reduce_sides(1)
    reduce_corner(2)
    cross_heads(3)
    compute(3)
    finish(1)
    reduce_sides(2)
    ready_heads()
    attend(0)
    reduce_corner(3)
    attend(1)
    finish(2)
    reduce_sides(3)
    attend(2)
    finish(3)
    attend(3)
    send_attended()
    for copy in homed:
        copy.wait_recv()
    gathered = returned[...].reshape(own_count, model_width)
    moe_out[...] = jnp.dot(slots, gathered, preferred_element_type=jnp.float32).astype(
        jnp.bfloat16
    )
    for copy in back:
        copy.wait_recv()
    for number in range(groups):
        columns = slice(number * head_width, (number + 1) * head_width)
        attn_out[:, columns] = jnp.where(
            plane == number, heads_done[number], heads_back[number]
        )
    copies.drain()


def fused_local(
    queries,
    keys,
    values,
    lambdas,
    head_gain,
    moe_input,
    ffn_gain,
    group_router,
    expert_router,
    routes,
    w_gate,
    w_up,
    w_down,
):
    groups = group_router.shape[1]
    token_block, width = queries.shape
    head_width = width // groups
    model_width = moe_input.shape[1]
    own_count = moe_input.shape[0] // lax.axis_size("tp")
    hidden_width = w_gate.shape[2]
    chunk = own_count // groups
    router = jnp.concatenate([group_router, expert_router], axis=1)
    router = jnp.pad(router, ((0, 0), (0, -router.shape[1] % 128)))
    bf16, f32 = jnp.bfloat16, jnp.float32
    vmem = pl.BlockSpec(memory_space=pltpu.VMEM)
    smem = pl.BlockSpec(memory_space=pltpu.SMEM)
    hbm = pl.BlockSpec(memory_space=pl.ANY)
    copy_count = 3 + 9 + 8 * groups + 5 * groups + 3 + 8 + 3
    blocks = 2 * groups
    return pl.pallas_call(
        functools.partial(fused_kernel, groups, (head_width // 2) ** -0.5),
        out_shape=(
            jax.ShapeDtypeStruct((token_block, width), bf16),
            jax.ShapeDtypeStruct((own_count, model_width), bf16),
        ),
        in_specs=[hbm, hbm, hbm, smem, vmem, hbm, vmem, vmem, vmem, hbm, hbm, hbm],
        out_specs=(vmem, vmem),
        scratch_shapes=[
            pltpu.VMEM((own_count, model_width), bf16),
            pltpu.VMEM((groups, chunk, model_width), bf16),
            pltpu.VMEM((groups, 8 * chunk, model_width), bf16),
            pltpu.VMEM((model_width, hidden_width), bf16),
            pltpu.VMEM((model_width, hidden_width), bf16),
            pltpu.VMEM((hidden_width, model_width), bf16),
            pltpu.VMEM((groups, 4 * chunk, model_width), bf16),
            pltpu.VMEM((groups, 4 * chunk, model_width), bf16),
            pltpu.VMEM((groups, 4 * chunk, model_width), f32),
            pltpu.VMEM((groups, chunk, model_width), bf16),
            pltpu.VMEM((groups, chunk, model_width), bf16),
            pltpu.VMEM((groups, 2 * chunk, model_width), bf16),
            pltpu.VMEM((groups, 2 * chunk, model_width), bf16),
            pltpu.VMEM((groups, chunk, model_width), bf16),
            pltpu.VMEM((groups, chunk, model_width), bf16),
            pltpu.VMEM((groups, token_block, head_width), bf16),
            pltpu.VMEM((blocks, token_block, head_width), bf16),
            pltpu.VMEM((blocks, token_block, head_width), bf16),
            pltpu.VMEM((groups, token_block, head_width), bf16),
            pltpu.VMEM((groups, token_block, head_width), bf16),
            pltpu.SemaphoreType.DMA((7,)),
            pltpu.SemaphoreType.DMA((copy_count,)),
            pltpu.SemaphoreType.DMA((copy_count,)),
        ],
        compiler_params=pltpu.CompilerParams(
            collective_id=0, has_side_effects=True, vmem_limit_bytes=62_000_000
        ),
    )(
        queries,
        keys,
        values,
        lambdas,
        head_gain[None, :],
        moe_input,
        ffn_gain[None, :],
        router,
        routes,
        w_gate,
        w_up,
        w_down,
    )


def chosen_local(*arguments):
    queries, lambdas = arguments[0], arguments[3]
    moe_input, group_router, expert_router = arguments[5], arguments[7], arguments[8]
    groups, experts = group_router.shape[1], expert_router.shape[1]
    fits = (
        experts == 2 * groups
        and lax.axis_size("ep") == experts
        and lax.axis_size("tp") == 4
        and groups == 4
        and lambdas.shape[0] == groups
        and queries.shape[1] == groups * 128
        and moe_input.shape[0] // 4 == 128
    )
    return fused_local(*arguments) if fits else local(*arguments)


def solution(mesh):
    in_specs = (
        P("ep", "tp"),
        P("ep", "tp"),
        P("ep", "tp"),
        P("tp"),
        P(),
        P("ep", None),
        P(),
        P(),
        P(),
        P("ep", None),
        P("ep", None, "tp"),
        P("ep", None, "tp"),
        P("ep", "tp", None),
    )
    out_specs = (P("ep", "tp"), P(("ep", "tp"), None))
    return jax.shard_map(
        chosen_local, mesh=mesh, in_specs=in_specs, out_specs=out_specs, check_vma=False)
```

```python
import functools
import math

import jax
import jax.numpy as jnp
from jax import lax
from jax.experimental import pallas as pl
from jax.experimental.pallas import tpu as pltpu
from jax.sharding import PartitionSpec as P

norm_eps = 1e-06
masked_score = -1e30


def rms_scaled(rows, gain):
    widened = rows.astype(jnp.float32)
    return (
        widened * lax.rsqrt(jnp.mean(widened * widened, axis=-1, keepdims=True) + norm_eps) * gain
    )


def score_block(query_heads, key_rows, score_scale):
    key_heads = key_rows.reshape(key_rows.shape[0], query_heads.shape[1], 2, query_heads.shape[3])
    return (
        jnp.einsum("qhmd,khmd->hmqk", query_heads, key_heads, preferred_element_type=jnp.float32)
        * score_scale
    )


def route_gates(normed, own_routes, group_router, expert_router):
    group_count = group_router.shape[1]
    expert_count = expert_router.shape[1]
    group_logits = jnp.dot(normed, group_router, preferred_element_type=jnp.float32)
    expert_logits = jnp.dot(normed, expert_router, preferred_element_type=jnp.float32)
    chosen = own_routes[:, 0] // (expert_count // group_count)
    group_mask = jnp.arange(group_count, dtype=jnp.int32)[None, :] == chosen[:, None]
    own_logit = jnp.sum(jnp.where(group_mask, group_logits, 0.0), axis=-1, keepdims=True)
    group_share = 1.0 / jnp.sum(jnp.exp(group_logits - own_logit), axis=-1)
    expert_mask = jnp.arange(expert_count, dtype=jnp.int32)[None, None, :] == own_routes[:, :, None]
    picked = jnp.sum(jnp.where(expert_mask, expert_logits[:, None, :], 0.0), axis=-1)
    return group_share[:, None] * jax.nn.sigmoid(picked - picked[:, ::-1])


def slot_places(own_routes, expert_count, capacity):
    flat_routes = own_routes.reshape(-1)
    one_hot = (flat_routes[:, None] == jnp.arange(expert_count, dtype=jnp.int32)[None, :]).astype(
        jnp.int32
    )
    earlier = jnp.cumsum(one_hot, axis=0) - one_hot
    return flat_routes * capacity + jnp.sum(earlier * one_hot, axis=1)


def dispatch_rows(normed_rows, own_routes, expert_count, capacity):
    places = slot_places(own_routes, expert_count, capacity)
    owners = jnp.arange(places.shape[0], dtype=jnp.int32) // 2
    holder = jnp.zeros((expert_count * capacity,), jnp.int32).at[places].set(owners)
    return normed_rows[holder].reshape(expert_count, capacity, normed_rows.shape[1])


def local(
    queries,
    keys,
    values,
    lambdas,
    head_gain,
    moe_input,
    ffn_gain,
    group_router,
    expert_router,
    routes,
    w_gate,
    w_up,
    w_down,
):
    query_count = queries.shape[0]
    heads_here = lambdas.shape[0]
    value_width = values.shape[1] // heads_here
    qk_width = queries.shape[1] // (2 * heads_here)
    query_heads = queries.reshape(query_count, heads_here, 2, qk_width)
    score_scale = qk_width ** (-0.5)
    query_first = lax.axis_index("ep") * query_count
    query_pos = query_first + jnp.arange(query_count, dtype=jnp.int32)
    query_last = query_first + query_count - 1
    stats_start = (
        jnp.full((heads_here, 2, query_count), masked_score, jnp.float32),
        jnp.zeros((heads_here, 2, query_count), jnp.float32),
    )
    key_shard = lax.all_gather(keys, "ep", axis=0, tiled=True)
    block_rows = math.gcd(key_shard.shape[0], 512)

    def stats_sweep_step(number, current):
        offset = number * block_rows

        def stats_compute(running):
            maxima, totals = running
            key_pos = offset + jnp.arange(block_rows, dtype=jnp.int32)
            allowed = key_pos[None, :] <= query_pos[:, None]
            key_block = lax.dynamic_slice_in_dim(key_shard, offset, block_rows, 0)
            scores = jnp.where(
                allowed, score_block(query_heads, key_block, score_scale), masked_score
            )
            new_max = jnp.maximum(maxima, jnp.max(scores, axis=-1))
            weights = jnp.where(allowed, jnp.exp(scores - new_max[..., None]), 0.0)
            return (new_max, totals * jnp.exp(maxima - new_max) + jnp.sum(weights, axis=-1))

        return lax.cond(offset <= query_last, stats_compute, lambda running: running, current)

    maxima, totals = lax.fori_loop(
        0, key_shard.shape[0] // block_rows, stats_sweep_step, stats_start
    )
    value_key_shard = lax.all_gather(keys, "ep", axis=0, tiled=True)
    value_shard = lax.all_gather(values, "ep", axis=0, tiled=True)
    value_block_rows = math.gcd(value_key_shard.shape[0], 512)

    def value_sweep_step(number, current):
        offset = number * value_block_rows

        def value_compute(running):
            key_pos = offset + jnp.arange(value_block_rows, dtype=jnp.int32)
            allowed = key_pos[None, :] <= query_pos[:, None]
            key_block = lax.dynamic_slice_in_dim(value_key_shard, offset, value_block_rows, 0)
            scores = score_block(query_heads, key_block, score_scale)
            shares = (
                jnp.where(allowed, jnp.exp(scores - maxima[..., None]), 0.0) / totals[..., None]
            )
            mixed = (shares[:, 0] - lambdas[:, None, None] * shares[:, 1]).astype(jnp.bfloat16)
            value_rows = lax.dynamic_slice_in_dim(value_shard, offset, value_block_rows, 0).reshape(
                value_block_rows, heads_here, value_width
            )
            return running + jnp.einsum(
                "hqk,khd->hqd", mixed, value_rows, preferred_element_type=jnp.float32
            )

        return lax.cond(offset <= query_last, value_compute, lambda running: running, current)

    heads_out = lax.fori_loop(
        0,
        value_key_shard.shape[0] // value_block_rows,
        value_sweep_step,
        jnp.zeros((heads_here, query_count, value_width), jnp.float32),
    )
    attn_out = rms_scaled(heads_out, head_gain).astype(jnp.bfloat16)
    attn_out = attn_out.transpose(1, 0, 2).reshape(query_count, heads_here * value_width)
    tp_count = lax.axis_size("tp")
    tp_index = lax.axis_index("tp")
    own_count = routes.shape[0] // tp_count
    expert_count = expert_router.shape[1]
    capacity = 2 * own_count // expert_count
    model_width = moe_input.shape[1]
    own_routes = lax.dynamic_slice_in_dim(routes, tp_index * own_count, own_count, 0)
    gate_local = w_gate[0]
    up_local = w_up[0]
    down_local = w_down[0]
    own_input = lax.dynamic_slice_in_dim(moe_input, tp_index * own_count, own_count, 0)
    normed = rms_scaled(own_input, ffn_gain).astype(jnp.bfloat16)
    packed = dispatch_rows(normed, own_routes, expert_count, capacity)
    arrived = lax.all_to_all(packed, "ep", split_axis=0, concat_axis=0, tiled=True)
    arrived_rows = lax.all_gather(arrived.reshape(-1, model_width), "tp", axis=0, tiled=True)
    gate_part = jnp.dot(arrived_rows, gate_local, preferred_element_type=jnp.float32)
    up_part = jnp.dot(arrived_rows, up_local, preferred_element_type=jnp.float32)
    hidden = (jax.nn.silu(gate_part) * up_part).astype(jnp.bfloat16)
    summed = lax.psum_scatter(
        jnp.dot(hidden, down_local, preferred_element_type=jnp.float32).astype(jnp.bfloat16),
        "tp",
        scatter_dimension=0,
        tiled=True,
    )
    homed = lax.all_to_all(
        summed.reshape(expert_count, capacity, model_width),
        "ep",
        split_axis=0,
        concat_axis=0,
        tiled=True,
    )
    places = slot_places(own_routes, expert_count, capacity)
    returned = homed.reshape(expert_count * capacity, model_width)[places].reshape(
        own_count, 2, model_width
    )
    gates = route_gates(normed, own_routes, group_router, expert_router)
    moe_out = jnp.sum(returned.astype(jnp.float32) * gates[..., None], axis=1).astype(jnp.bfloat16)
    return (attn_out, moe_out)


class Copies:
    def __init__(self, send_sems, recv_sems):
        self.send_sems = send_sems
        self.recv_sems = recv_sems
        self.made = []

    def new(self, source, target, device):
        number = len(self.made)
        copy = pltpu.make_async_remote_copy(
            src_ref=source,
            dst_ref=target,
            send_sem=self.send_sems.at[number],
            recv_sem=self.recv_sems.at[number],
            device_id=device,
            device_id_type=pl.DeviceIdType.MESH,
        )
        copy.start()
        self.made.append(copy)
        return copy

    def drain(self):
        for copy in self.made:
            copy.wait_send()


def fused_kernel(
    groups,
    score_scale,
    queries,
    keys,
    values,
    lambdas,
    head_gain,
    moe_input,
    ffn_gain,
    group_router,
    expert_router,
    routes,
    w_gate,
    w_up,
    w_down,
    attn_out,
    moe_out,
    own_rows,
    packed,
    rows,
    gate_w,
    up_w,
    down_w,
    half_out,
    half_in,
    sums,
    corner_out,
    corner_in,
    side_out,
    side_in,
    done,
    returned,
    q_all,
    k_all,
    v_all,
    heads_done,
    heads_back,
    router,
    local_sems,
    send_sems,
    recv_sems,
    back_send_sems,
    back_recv_sems,
):
    own_count, model_width = own_rows.shape
    expert_first = 16
    chunk = own_count // groups
    halves = [chunk if step % 2 == 0 else chunk // 2 for step in range(groups)]
    token_block, head_width = q_all.shape[1:]
    ep = lax.axis_index("ep")
    tp = lax.axis_index("tp")
    plane, member = ep // 2, ep % 2
    row, core = tp // 2, tp % 2
    member_peer = (plane * 2 + (1 - member), tp)
    row_peer = (ep, (1 - row) * 2 + core)
    core_peer = (ep, row * 2 + (1 - core))
    high, low = plane // 2, plane % 2
    ahead = [
        (high + step // 2) % 2 * 2 + (low + step % 2) % 2 for step in range(groups)
    ]
    behind = ahead

    def at_plane(number):
        return (number * 2 + member, tp)

    def head_columns(ref, number):
        return ref.at[:, pl.ds(pl.multiple_of(number * head_width, head_width), head_width)]

    loads = []
    for source, target in (
        (moe_input.at[pl.ds(pl.multiple_of(tp * own_count, own_count), own_count)], own_rows),
        (head_columns(queries, plane), q_all.at[plane]),
        (head_columns(keys, plane), k_all.at[ep]),
        (head_columns(values, plane), v_all.at[ep]),
        (w_gate.at[0], gate_w),
        (w_up.at[0], up_w),
        (w_down.at[0], down_w),
    ):
        load = pltpu.make_async_copy(source, target, local_sems.at[len(loads)])
        load.start()
        loads.append(load)

    barrier = pltpu.get_barrier_semaphore()
    partners = [member_peer, row_peer, core_peer] + [at_plane(p) for p in ahead[1:]]
    for partner in partners:
        pl.semaphore_signal(
            barrier, inc=1, device_id=partner, device_id_type=pl.DeviceIdType.MESH
        )

    lead = routes[0:1, pl.ds(pl.multiple_of(tp * own_count, own_count), own_count)]
    lane = lax.broadcasted_iota(jnp.int32, (own_count, own_count), 1)
    sub = lax.broadcasted_iota(jnp.int32, (own_count, own_count), 0)
    sub_group = jnp.zeros_like(sub)
    for step in range(groups):
        sub_group = jnp.where(sub == step, ahead[step], sub_group)
    in_group = (lead >= sub_group * 2) & (lead < sub_group * 2 + 2) & (sub < groups)
    one_hot = jnp.where(in_group, 1.0, 0.0)
    before = jnp.where(sub < lane, 1.0, 0.0).astype(jnp.bfloat16)
    earlier = jnp.dot(one_hot.astype(jnp.bfloat16), before, preferred_element_type=jnp.float32)
    sub_start = (sub * chunk).astype(jnp.float32)
    place = jnp.sum(one_hot * (earlier + sub_start), axis=0, keepdims=True)
    slots = jnp.where(place == sub.astype(jnp.float32), 1.0, 0.0).astype(jnp.bfloat16)
    router[...] = jnp.zeros_like(router)
    router[0:groups, :] = group_router[...]
    router[expert_first : expert_first + 2 * groups, :] = expert_router[...]

    loads[0].wait()
    widened = own_rows[...].astype(jnp.float32)
    normed = (
        widened
        * lax.rsqrt(jnp.mean(widened * widened, axis=-1, keepdims=True) + norm_eps)
        * ffn_gain[...]
    ).astype(jnp.bfloat16)
    by_group = jnp.dot(slots, normed, preferred_element_type=jnp.float32).astype(jnp.bfloat16)
    rows[0, 0:chunk, :] = by_group[0:chunk]
    for step in range(1, groups):
        packed[step] = by_group[step * chunk : (step + 1) * chunk]

    pl.semaphore_wait(barrier, len(partners))
    copies = Copies(send_sems, recv_sems)

    def slot(step, number):
        return rows.at[step, pl.ds(number * chunk, chunk)]

    arriving = [None] * groups
    for step in range(1, groups):
        arriving[step] = copies.new(packed.at[step], slot(step, 0), at_plane(ahead[step]))
    kv_arriving = [None] * groups
    q_arriving = []

    def send_heads(step):
        target = at_plane(ahead[step])
        kv_arriving[step] = [
            copies.new(head_columns(keys, ahead[step]), k_all.at[ep], target),
            copies.new(head_columns(values, ahead[step]), v_all.at[ep], target),
        ]
        q_arriving.append(
            copies.new(head_columns(queries, ahead[step]), q_all.at[plane], target)
        )

    first = [None] * groups
    second = [None] * groups
    third = [None] * groups
    crossed = [None] * groups
    corner = [None] * groups
    sides = [None] * groups
    homed = []
    kv_crossed = []

    def spread(step):
        if arriving[step] is not None:
            arriving[step].wait_recv()
        first[step] = [
            copies.new(slot(step, 0), slot(step, 1), member_peer),
            copies.new(slot(step, 0), slot(step, 2), row_peer),
        ]
        third[step] = [copies.new(slot(step, 0), slot(step, groups_in_half), core_peer)]

    def forward(step):
        half = halves[step]
        first[step][0].wait_recv()
        second[step] = [
            copies.new(
                rows.at[step, pl.ds(chunk, half)], rows.at[step, pl.ds(3 * chunk, half)], row_peer
            )
        ]
        third[step].append(copies.new(slot(step, 1), slot(step, 5), core_peer))
        first[step][1].wait_recv()
        if half < chunk:
            second[step].append(
                copies.new(
                    rows.at[step, pl.ds(2 * chunk + half, chunk - half)],
                    rows.at[step, pl.ds(3 * chunk + half, chunk - half)],
                    member_peer,
                )
            )
        third[step].append(copies.new(slot(step, 2), slot(step, 6), core_peer))

    def pass_corner(step):
        for copy in second[step]:
            copy.wait_recv()
        third[step].append(copies.new(slot(step, 3), slot(step, 7), core_peer))

    def compute(step):
        for copy in third[step]:
            copy.wait_recv()
        block = rows[step]
        logits = lax.dot_general(
            block, router[...], (((1,), (1,)), ((), ())), preferred_element_type=jnp.float32
        )
        column = lax.broadcasted_iota(jnp.int32, logits.shape, 1)

        def pick(number):
            return jnp.sum(jnp.where(column == number, logits, 0.0), axis=1, keepdims=True)

        own_group = pick(plane)
        terms = jnp.where(column < groups, jnp.exp(logits - own_group), 0.0)
        share = 1.0 / jnp.sum(jnp.where(column < groups, terms, 0.0), axis=1, keepdims=True)
        gap = pick(expert_first + ep) - pick(expert_first + plane * 2 + (1 - member))
        gates = share / (1.0 + jnp.exp(-gap))
        gate_part = jnp.dot(block, gate_w[...], preferred_element_type=jnp.float32)
        up_part = jnp.dot(block, up_w[...], preferred_element_type=jnp.float32)
        hidden = (gate_part / (1.0 + jnp.exp(-gate_part)) * up_part).astype(jnp.bfloat16)
        out = jnp.dot(hidden, down_w[...], preferred_element_type=jnp.float32) * gates
        half_out[step] = out[4 * chunk :].astype(jnp.bfloat16)
        sums[step] = out[: 4 * chunk]
        crossed[step] = copies.new(half_out.at[step], half_in.at[step], core_peer)

    def reduce_corner(step):
        crossed[step].wait_recv()
        total = sums[step] + half_in[step].astype(jnp.float32)
        sums[step] = total
        corner_out[step] = total[3 * chunk :].astype(jnp.bfloat16)
        half = halves[step]
        corner[step] = [
            copies.new(
                corner_out.at[step, pl.ds(0, half)], corner_in.at[step, pl.ds(0, half)], row_peer
            )
        ]
        if half < chunk:
            corner[step].append(
                copies.new(
                    corner_out.at[step, pl.ds(half, chunk - half)],
                    corner_in.at[step, pl.ds(half, chunk - half)],
                    member_peer,
                )
            )

    def reduce_sides(step):
        for copy in corner[step]:
            copy.wait_recv()
        half = halves[step]
        added = corner_in[step].astype(jnp.float32)
        total = sums[step]
        side_out[step, 0:half, :] = (total[chunk : chunk + half] + added[:half]).astype(
            jnp.bfloat16
        )
        side_out[step, half : half + chunk, :] = total[chunk + half : 2 * chunk + half].astype(
            jnp.bfloat16
        )
        if half < chunk:
            side_out[step, half + chunk :, :] = (
                total[2 * chunk + half : 3 * chunk] + added[half:]
            ).astype(jnp.bfloat16)
        sides[step] = [
            copies.new(
                side_out.at[step, pl.ds(0, chunk)], side_in.at[step, pl.ds(0, chunk)], member_peer
            ),
            copies.new(
                side_out.at[step, pl.ds(chunk, chunk)],
                side_in.at[step, pl.ds(chunk, chunk)],
                row_peer,
            ),
        ]

    def finish(step):
        for copy in sides[step]:
            copy.wait_recv()
        arrived = side_in[step].astype(jnp.float32)
        total = (sums[step][:chunk] + arrived[:chunk] + arrived[chunk:]).astype(jnp.bfloat16)
        if step == 0:
            returned[0] = total
        else:
            done[step] = total
            homed.append(copies.new(done.at[step], returned.at[step], at_plane(behind[step])))

    def cross_heads(step):
        if step == 0:
            loads[2].wait()
            loads[3].wait()
        else:
            for copy in kv_arriving[step]:
                copy.wait_recv()
        block = behind[step] * 2 + member
        kv_crossed.append(copies.new(k_all.at[block], k_all.at[block], member_peer))
        kv_crossed.append(copies.new(v_all.at[block], v_all.at[block], member_peer))

    def ready_heads():
        loads[1].wait()
        for copy in q_arriving + kv_crossed:
            copy.wait_recv()

    weight = lambdas[plane]
    factor = score_scale * math.log2(math.e)

    def attend(number):
        query = q_all[number]
        lanes = lax.broadcasted_iota(jnp.int32, query.shape, 1)
        nothing = jnp.zeros_like(query)
        maps = [
            jnp.where(lanes < head_width // 2, query, nothing),
            jnp.where(lanes >= head_width // 2, query, nothing),
        ]
        ends = [2 * number, 2 * number + 2]
        parts = [(0, ends[0])] if number else []
        parts.append((ends[0], ends[1]))
        key_parts = [k_all[a:b].reshape((b - a) * token_block, head_width) for a, b in parts]
        value_parts = [v_all[a:b].reshape((b - a) * token_block, head_width) for a, b in parts]
        mixed = [None] * len(parts)
        for index, part_query in enumerate(maps):
            scores = [
                lax.dot_general(
                    part_query, k, (((1,), (1,)), ((), ())), preferred_element_type=jnp.float32
                )
                for k in key_parts
            ]
            at = lax.broadcasted_iota(jnp.int32, scores[-1].shape, 1)
            own = lax.broadcasted_iota(jnp.int32, scores[-1].shape, 0) + member * token_block
            scores[-1] = jnp.where(at <= own, scores[-1], masked_score)
            maxima = functools.reduce(
                jnp.maximum, [jnp.max(s, axis=1, keepdims=True) for s in scores]
            )
            terms = [jnp.exp2((s - maxima) * factor) for s in scores]
            total = sum(jnp.sum(t, axis=1, keepdims=True) for t in terms)
            share = 1.0 / total if index == 0 else -weight / total
            for place_number, t in enumerate(terms):
                piece = t * share
                if index:
                    piece = mixed[place_number] + piece
                mixed[place_number] = piece
        heads = sum(
            jnp.dot(w.astype(jnp.bfloat16), v, preferred_element_type=jnp.float32)
            for w, v in zip(mixed, value_parts)
        )
        scaled = (
            heads
            * lax.rsqrt(jnp.mean(heads * heads, axis=-1, keepdims=True) + norm_eps)
            * head_gain[...]
        )
        heads_done[number] = scaled.astype(jnp.bfloat16)

    def attended_copy(number, source):
        return pltpu.make_async_remote_copy(
            src_ref=heads_done.at[number],
            dst_ref=heads_back.at[source],
            send_sem=back_send_sems.at[number],
            recv_sem=back_recv_sems.at[source],
            device_id=at_plane(number),
            device_id_type=pl.DeviceIdType.MESH,
        )

    def attend_and_send(number):
        attend(number)

        @pl.when(plane != number)
        def _():
            attended_copy(number, plane).start()

    groups_in_half = 4
    spread(0)
    cross_heads(0)
    send_heads(1)
    send_heads(2)
    send_heads(3)
    spread(1)
    forward(0)
    spread(2)
    forward(1)
    pass_corner(0)
    cross_heads(1)
    spread(3)
    forward(2)
    pass_corner(1)
    for load in loads[4:]:
        load.wait()
    compute(1)
    forward(3)
    cross_heads(2)
    pass_corner(2)
    compute(2)
    reduce_corner(1)
    pass_corner(3)
    cross_heads(3)
    compute(3)
    reduce_corner(2)
    reduce_sides(1)
    compute(0)
    reduce_corner(3)
    reduce_sides(2)
    ready_heads()
    attend_and_send(0)
    attend_and_send(1)
    finish(1)
    reduce_corner(0)
    reduce_sides(3)
    attend_and_send(2)
    finish(2)
    reduce_sides(0)
    attend_and_send(3)
    finish(3)
    finish(0)
    for copy in homed:
        copy.wait_recv()
    gathered = returned[...].reshape(own_count, model_width)
    moe_out[...] = lax.dot_general(
        slots, gathered, (((0,), (0,)), ((), ())), preferred_element_type=jnp.float32
    ).astype(jnp.bfloat16)
    for number in range(groups):

        @pl.when(plane != number)
        def _(number=number):
            attended_copy(number, number).wait_recv()

    for number in range(groups):
        columns = slice(number * head_width, (number + 1) * head_width)
        attn_out[:, columns] = jnp.where(
            plane == number, heads_done[number], heads_back[number]
        )
    for number in range(groups):

        @pl.when(plane != number)
        def _(number=number):
            attended_copy(number, plane).wait_send()

    copies.drain()


def store_kernel(attn_in, moe_in, attn_out, moe_out, sems):
    pairs = ((attn_in, attn_out), (moe_in, moe_out))
    stores = [pltpu.make_async_copy(a, b, sems.at[n]) for n, (a, b) in enumerate(pairs)]
    for store in stores:
        store.start()
    for store in stores:
        store.wait()


def fused_local(
    queries,
    keys,
    values,
    lambdas,
    head_gain,
    moe_input,
    ffn_gain,
    group_router,
    expert_router,
    routes,
    w_gate,
    w_up,
    w_down,
):
    groups = group_router.shape[1]
    token_block, width = queries.shape
    head_width = width // groups
    model_width = moe_input.shape[1]
    own_count = moe_input.shape[0] // lax.axis_size("tp")
    hidden_width = w_gate.shape[2]
    chunk = own_count // groups
    bf16, f32 = jnp.bfloat16, jnp.float32
    vmem = pl.BlockSpec(memory_space=pltpu.VMEM)
    smem = pl.BlockSpec(memory_space=pltpu.SMEM)
    hbm = pl.BlockSpec(memory_space=pl.ANY)
    copy_count = 3 + 9 + 8 * groups + 5 * groups + 3 + 8 + 3
    blocks = 2 * groups
    results = pl.pallas_call(
        functools.partial(fused_kernel, groups, (head_width // 2) ** -0.5),
        out_shape=(
            jax.ShapeDtypeStruct((token_block, width), bf16),
            jax.ShapeDtypeStruct((own_count, model_width), bf16),
        ),
        in_specs=[hbm, hbm, hbm, smem, vmem, hbm] + [vmem] * 4 + [hbm] * 3,
        out_specs=(vmem, vmem),
        scratch_shapes=[
            pltpu.VMEM((own_count, model_width), bf16),
            pltpu.VMEM((groups, chunk, model_width), bf16),
            pltpu.VMEM((groups, 8 * chunk, model_width), bf16),
            pltpu.VMEM((model_width, hidden_width), bf16),
            pltpu.VMEM((model_width, hidden_width), bf16),
            pltpu.VMEM((hidden_width, model_width), bf16),
            pltpu.VMEM((groups, 4 * chunk, model_width), bf16),
            pltpu.VMEM((groups, 4 * chunk, model_width), bf16),
            pltpu.VMEM((groups, 4 * chunk, model_width), f32),
            pltpu.VMEM((groups, chunk, model_width), bf16),
            pltpu.VMEM((groups, chunk, model_width), bf16),
            pltpu.VMEM((groups, 2 * chunk, model_width), bf16),
            pltpu.VMEM((groups, 2 * chunk, model_width), bf16),
            pltpu.VMEM((groups, chunk, model_width), bf16),
            pltpu.VMEM((groups, chunk, model_width), bf16),
            pltpu.VMEM((groups, token_block, head_width), bf16),
            pltpu.VMEM((blocks, token_block, head_width), bf16),
            pltpu.VMEM((blocks, token_block, head_width), bf16),
            pltpu.VMEM((groups, token_block, head_width), bf16),
            pltpu.VMEM((groups, token_block, head_width), bf16),
            pltpu.VMEM((128, model_width), bf16),
            pltpu.SemaphoreType.DMA((7,)),
            pltpu.SemaphoreType.DMA((copy_count,)),
            pltpu.SemaphoreType.DMA((copy_count,)),
            pltpu.SemaphoreType.DMA((groups,)),
            pltpu.SemaphoreType.DMA((groups,)),
        ],
        compiler_params=pltpu.CompilerParams(
            collective_id=0, has_side_effects=True, vmem_limit_bytes=62_000_000
        ),
    )(
        queries,
        keys,
        values,
        lambdas,
        head_gain[None, :],
        moe_input,
        ffn_gain[None, :],
        group_router.T,
        expert_router.T,
        routes.T,
        w_gate,
        w_up,
        w_down,
    )
    return pl.pallas_call(
        store_kernel,
        out_shape=tuple(jax.ShapeDtypeStruct(r.shape, r.dtype) for r in results),
        in_specs=[vmem, vmem],
        out_specs=(hbm, hbm),
        scratch_shapes=[pltpu.SemaphoreType.DMA((2,))],
    )(*results)


def chosen_local(*arguments):
    queries, lambdas = arguments[0], arguments[3]
    moe_input, group_router, expert_router = arguments[5], arguments[7], arguments[8]
    groups, experts = group_router.shape[1], expert_router.shape[1]
    fits = (
        experts == 2 * groups
        and lax.axis_size("ep") == experts
        and lax.axis_size("tp") == 4
        and groups == 4
        and lambdas.shape[0] == groups
        and queries.shape[1] == groups * 128
        and moe_input.shape[0] // 4 == 128
    )
    return fused_local(*arguments) if fits else local(*arguments)


def solution(mesh):
    in_specs = (
        P("ep", "tp"),
        P("ep", "tp"),
        P("ep", "tp"),
        P("tp"),
        P(),
        P("ep", None),
        P(),
        P(),
        P(),
        P("ep", None),
        P("ep", None, "tp"),
        P("ep", None, "tp"),
        P("ep", "tp", None),
    )
    out_specs = (P("ep", "tp"), P(("ep", "tp"), None))
    return jax.shard_map(
        chosen_local, mesh=mesh, in_specs=in_specs, out_specs=out_specs, check_vma=False)
```
